32 devices in a mesh: rep: 4 (over z), fs: 4 (over y, x), tp: 2 (over core).
Axes of the slice: x: 2, y: 2, z: 4, core: 2. Of those that a mesh axis runs over, the one named last changes fastest.
Arguments:
- tokens: bfloat16 [4096, 2048], P(('rep', 'fs', 'tp')), may hold values from -6 to 6
- cotangent: bfloat16 [4096, 2048], P(('rep', 'fs', 'tp')), may hold values from -6 to 6
- gate_weight: bfloat16 [2048, 3072], P(None, 'fs'), may hold values from -0.125 to 0.125
- up_weight: bfloat16 [2048, 3072], P(None, 'fs'), may hold values from -0.125 to 0.125
- down_weight_t: bfloat16 [2048, 3072], P(None, 'fs'), may hold values from -0.109375 to 0.109375
Outputs:
- input_grad: bfloat16 [4096, 2048], P(('rep', 'fs', 'tp'))
- gate_grad: float32 [2048, 3072], P(('rep', 'tp'), 'fs')
- up_grad: float32 [2048, 3072], P(('rep', 'tp'), 'fs')
- down_grad: float32 [2048, 3072], P(('rep', 'tp'), 'fs')
The draws below stay inside these ranges and needn't reach their ends.
All inputs are finite; a program needn't handle non-finite values.
Results may differ from the reference program's by a relative error of at most 0.012.
Values may be sent and summed in bfloat16 or wider, within the bound.
A program may use at most 128 MiB of HBM per device.

```python
import jax
import jax.numpy as jnp
from jax import lax

D = 2048
FF = 3072
TOKENS = 4096
N_REP = 4
N_FS = 4


def raised(result, rng, source, target, blocks, factor):
    def block_of(axis_at):
        return (jnp.arange(result.shape[axis_at]) // (result.shape[axis_at] // blocks)).reshape((-1,) + (1,) * (result.ndim - 1 - axis_at))

    first = jax.random.permutation(rng, blocks)[block_of(target)]
    other_side = (block_of(target) + blocks // 2) % blocks
    return jnp.where((block_of(source) == first) | (block_of(source) == other_side), factor * result, result)


def block_levels(rng, shape, shards, low, top_value):
    def one(dim, shards_of):
        heights = jax.random.uniform(jax.random.fold_in(jax.random.fold_in(rng, 6), dim), (shards_of,), jnp.float32, low / len(shards), top_value / len(shards))
        return jnp.repeat(jnp.exp(heights), shape[dim] // shards_of).reshape((-1,) + (1,) * (len(shape) - dim - 1))

    loudness = one(*shards[0])
    for cut in shards[1:]:
        loudness = loudness * one(*cut)
    return loudness


def gaussian(key, extent, width, limit, split=(), kind=jnp.bfloat16):
    loudness = block_levels(key, extent, split, -0.22, 0.18) if split else 1.0
    result = jax.random.normal(key, extent, jnp.float32) * width * loudness
    return jnp.minimum(jnp.maximum(result, -limit), limit).astype(kind)


def noise_with(key, dims, width, most, pieces, heavy, held_as=jnp.bfloat16):
    values = width * jax.random.normal(key, dims, jnp.float32)
    if pieces:
        values = values * block_levels(key, dims, pieces, -0.22, 0.18)
    return jnp.clip(raised(values, jax.random.fold_in(key, 3), *heavy), -most, most).astype(held_as)


def setup_inputs(seed: int = 0) -> dict:
    arg_keys = jax.random.split(jax.random.key(seed), 6)
    tokens = noise_with(arg_keys[0], (TOKENS, D), 1.0, 6.0, ((0, 32),), (0, 1, 32, 2.75))
    cotangent = noise_with(arg_keys[1], (TOKENS, D), 1.0, 6.0, ((0, 32),), (0, 1, 32, 2.75))
    gate_weight = gaussian(arg_keys[2], (D, FF), D ** -0.5, 0.125, ((1, 4),))
    up_weight = gaussian(arg_keys[3], (D, FF), D ** -0.5, 0.125, ((1, 4),))
    down_weight_t = gaussian(arg_keys[4], (D, FF), FF ** -0.5, 0.109375, ((1, 4),))
    return dict(tokens=tokens, cotangent=cotangent, gate_weight=gate_weight, up_weight=up_weight, down_weight_t=down_weight_t)


def reference(tokens, cotangent, gate_weight, up_weight, down_weight_t):
    row_block = TOKENS // N_REP
    hid_width = FF // N_FS
    gate_split = gate_weight.astype(jnp.float32).reshape(D, N_FS, hid_width)
    up_split = up_weight.astype(jnp.float32).reshape(D, N_FS, hid_width)

    def accumulate(totals, block_index):
        first_row = block_index * row_block
        tok_rows = lax.dynamic_slice_in_dim(tokens, first_row, row_block, 0)
        cot_rows = lax.dynamic_slice_in_dim(cotangent, first_row, row_block, 0)
        gate_pre = jnp.dot(tok_rows, gate_weight, preferred_element_type=jnp.float32)
        up_pre = jnp.dot(tok_rows, up_weight, preferred_element_type=jnp.float32)
        sig_gate = jax.nn.sigmoid(gate_pre)
        act_gate = gate_pre * sig_gate
        hidden = (act_gate * up_pre).astype(jnp.bfloat16)
        hid_grad = jnp.dot(cot_rows, down_weight_t, preferred_element_type=jnp.float32)
        gate_back = (hid_grad * up_pre * sig_gate * (1.0 + gate_pre * (1.0 - sig_gate))).astype(jnp.bfloat16)
        up_back = (hid_grad * act_gate).astype(jnp.bfloat16)
        partial_value = jnp.einsum("rnf,dnf->nrd", gate_back.astype(jnp.float32).reshape(row_block, N_FS, hid_width),
                             gate_split, precision=lax.Precision.HIGHEST)
        partial_value = partial_value + jnp.einsum("rnf,dnf->nrd", up_back.astype(jnp.float32).reshape(row_block, N_FS, hid_width),
                                       up_split, precision=lax.Precision.HIGHEST)
        rounded = lax.optimization_barrier(partial_value.astype(jnp.bfloat16))
        input_rows = jnp.sum(rounded.astype(jnp.float32), axis=0).astype(jnp.bfloat16)
        new_totals = (totals[0] + jnp.dot(tok_rows.T, gate_back, preferred_element_type=jnp.float32),
                      totals[1] + jnp.dot(tok_rows.T, up_back, preferred_element_type=jnp.float32),
                      totals[2] + jnp.dot(cot_rows.T, hidden, preferred_element_type=jnp.float32))
        return new_totals, input_rows

    zeros = jnp.zeros((D, FF), jnp.float32)
    totals, input_blocks = lax.scan(accumulate, (zeros, zeros, zeros), jnp.arange(N_REP, dtype=jnp.int32))
    grad_scale = float(TOKENS) ** -0.5
    return (input_blocks.reshape(TOKENS, D), totals[0] * grad_scale, totals[1] * grad_scale, totals[2] * grad_scale)
```

```python
import functools

import jax
import jax.numpy as jnp
from jax import lax
from jax.experimental import pallas as pl
from jax.experimental.pallas import tpu as pltpu
from jax.sharding import PartitionSpec as P

MESH = pl.DeviceIdType.MESH
F32 = jnp.float32
BF16 = jnp.bfloat16


def tile_of(size, want=256):
    return want if size % want == 0 else size


def kernel(
    n_rep, n_tp, grad_scale,
    tok_hbm, cot_hbm, gw_hbm, uw_hbm, dw_hbm,
    igrad, ggrad, ugrad, dgrad,
    tok, cot, gw, uw, dw, tok_t, cot_t, gb, ub, hd, part, part_in, out_buf, in_buf,
    load_sem, g_send, g_recv, c_send, c_recv, p_send, p_recv, r_send, r_recv,
):
    slots, rows, features = tok.shape
    hidden = gb.shape[1]
    span = features // (n_rep * n_tp)
    half = hidden // 2
    me_r = lax.axis_index("rep")
    f = lax.axis_index("fs")
    t = lax.axis_index("tp")
    side = f + 1 - 2 * (f % 2)
    up = (f + 2) % 4
    diag = (side + 2) % 4
    peers = (None, side, up, diag)
    right = (me_r + 1) % n_rep
    left = (me_r + n_rep - 1) % n_rep
    twin = 1 - t

    def local(src, dst, i):
        return pltpu.make_async_copy(src, dst, load_sem.at[i])

    loads = [
        local(tok_hbm, tok.at[0], 0),
        local(cot_hbm, cot.at[0], 1),
        local(gw_hbm, gw, 2),
        local(uw_hbm, uw, 3),
        local(dw_hbm, dw, 4),
    ]
    for c in loads:
        c.start()

    barrier = pltpu.get_barrier_semaphore()
    targets = [{"fs": side}, {"fs": up}, {"fs": diag}, {"rep": right}, {"rep": left}, {"tp": twin}]
    for d in targets:
        pl.semaphore_signal(barrier, inc=1, device_id=d, device_id_type=MESH)
    pl.semaphore_wait(barrier, len(targets))

    def remote(src, dst, ss, rs, dev):
        return pltpu.make_async_remote_copy(
            src_ref=src, dst_ref=dst, send_sem=ss, recv_sem=rs, device_id=dev, device_id_type=MESH
        )

    def gather(i, src, dst, dev):
        return remote(src, dst, g_send.at[i], g_recv.at[i], {"fs": dev})

    cot_x = gather(0, cot_hbm, cot.at[1], side)
    tok_y = gather(1, tok_hbm, tok.at[2], up)
    tok_x = gather(2, tok_hbm, tok.at[1], side)
    cot_y = gather(3, cot_hbm, cot.at[2], up)
    tok_d = gather(4, tok.at[2], tok.at[3], side)
    cot_d = gather(5, cot.at[1], cot.at[3], up)
    for c in (cot_x, tok_y, tok_x, cot_y):
        c.start()

    def cross(k, i, src, dst):
        return remote(src, dst, c_send.at[k, i], c_recv.at[k, i], {"tp": twin})

    def crossings(k):
        here, there = slice(k * rows, (k + 1) * rows), slice((slots + k) * rows, (slots + k + 1) * rows)
        return [
            cross(k, 0, tok_t.at[:, here], tok_t.at[:, there]),
            cross(k, 1, cot_t.at[:, here], cot_t.at[:, there]),
            cross(k, 2, gb.at[here], gb.at[there]),
            cross(k, 3, ub.at[here], ub.at[there]),
            cross(k, 4, hd.at[here], hd.at[there]),
        ]

    def turn(k, src, dst):
        width = tile_of(features)

        @pl.loop(0, features // width)
        def _(j):
            piece = pl.ds(pl.multiple_of(j * width, width), width)
            dst[piece, k * rows:(k + 1) * rows] = src[k, :, piece].T

    def forward(k):
        width = tile_of(hidden)
        here = slice(k * rows, (k + 1) * rows)

        @pl.loop(0, hidden // width)
        def _(j):
            cols = pl.ds(pl.multiple_of(j * width, width), width)
            g = jnp.dot(tok[k], gw[:, cols], preferred_element_type=F32)
            u = jnp.dot(tok[k], uw[:, cols], preferred_element_type=F32)
            h = jnp.dot(cot[k], dw[:, cols], preferred_element_type=F32)
            sig = jax.nn.sigmoid(g)
            act = g * sig
            hd[here, cols] = (act * u).astype(BF16)
            gb[here, cols] = (h * u * sig * (1.0 + g * (1.0 - sig))).astype(BF16)
            ub[here, cols] = (h * act).astype(BF16)

    def handle(k):
        sends = crossings(k)
        turn(k, tok, tok_t)
        sends[0].start()
        turn(k, cot, cot_t)
        sends[1].start()
        forward(k)
        for c in sends[2:]:
            c.start()

    for c in loads:
        c.wait()
    handle(0)
    cot_x.wait_recv()
    cot_d.start()
    tok_y.wait_recv()
    tok_d.start()
    tok_x.wait_recv()
    handle(1)
    cot_y.wait_recv()
    handle(2)
    tok_d.wait_recv()
    cot_d.wait_recv()
    handle(3)
    for k in range(slots):
        for c in crossings(k):
            c.wait_recv()

    pairs = ((tok_t, gb), (tok_t, ub), (cot_t, hd))
    outs = (ggrad, ugrad, dgrad)

    def dest(way, s):
        if way == 0:
            return (me_r + 2 * n_rep - 1 - s) % n_rep
        return (me_r + 1 + s) % n_rep

    def piece(way, s, a):
        lhs, rhs = pairs[a]
        band = pl.ds(pl.multiple_of((dest(way, s) * n_tp + t) * span, span), span)
        return jnp.dot(lhs[band, :], rhs[:, way * half:(way + 1) * half], preferred_element_type=F32)

    def hop(way, s, a):
        return remote(
            out_buf.at[way, s, a], in_buf.at[way, s, a],
            r_send.at[way, s, a], r_recv.at[way, s, a],
            {"rep": right if way == 0 else left},
        )

    for a in range(3):
        for way in range(2):
            out_buf[way, 0, a] = piece(way, 0, a).astype(BF16)
            hop(way, 0, a).start()

    width = tile_of(features)
    across = (((1,), (1,)), ((), ()))

    @pl.loop(0, features // width)
    def _(j):
        band = pl.ds(pl.multiple_of(j * width, width), width)
        total = lax.dot_general(gb[0:slots * rows], gw[band, :], across, preferred_element_type=F32)
        total = total + lax.dot_general(ub[0:slots * rows], uw[band, :], across, preferred_element_type=F32)
        part[:, :, band] = total.astype(BF16).reshape(slots, rows, width)

    def give(k):
        return remote(part.at[k], part_in.at[k - 1], p_send.at[k - 1], p_recv.at[k - 1], {"fs": peers[k]})

    for k in (3, 1, 2):
        give(k).start()

    @pl.loop(1, n_rep - 1)
    def _(s):
        for a in range(3):
            for way in range(2):
                own = piece(way, s, a)
                hop(way, s - 1, a).wait_recv()
                out_buf[way, s, a] = (own + in_buf[way, s - 1, a].astype(F32)).astype(BF16)
                hop(way, s, a).start()

    for k in (1, 2, 3):
        give(k).wait_recv()
    igrad[...] = (
        part[0].astype(F32) + part_in[0].astype(F32) + part_in[1].astype(F32) + part_in[2].astype(F32)
    ).astype(BF16)

    for a in range(3):
        for way in range(2):
            own = piece(way, n_rep - 1, a)
            hop(way, n_rep - 2, a).wait_recv()
            outs[a][:, way * half:(way + 1) * half] = (
                own + in_buf[way, n_rep - 2, a].astype(F32)
            ) * grad_scale

    for c in (cot_x, tok_y, tok_x, cot_y, tok_d, cot_d):
        c.wait_send()
    for k in range(slots):
        for c in crossings(k):
            c.wait_send()
    for k in (1, 2, 3):
        give(k).wait_send()

    @pl.loop(0, n_rep - 1)
    def _(s):
        for a in range(3):
            for way in range(2):
                hop(way, s, a).wait_send()


def solution(mesh):
    n_rep, n_fs, n_tp = (mesh.shape[a] for a in ("rep", "fs", "tp"))
    assert n_fs == 4 and n_tp == 2 and n_rep > 2

    def on_device(tokens, cotangent, gate_weight, up_weight, down_weight_t):
        rows, features = tokens.shape
        hidden = gate_weight.shape[1]
        span = features // (n_rep * n_tp)
        both = n_tp * n_fs * rows
        hops = (2, n_rep - 1, 3)
        anywhere = pl.BlockSpec(memory_space=pl.ANY)
        vmem = pl.BlockSpec(memory_space=pltpu.VMEM)
        dma = pltpu.SemaphoreType.DMA
        grad = jax.ShapeDtypeStruct((span, hidden), F32)
        scale = float(rows * n_rep * n_fs * n_tp) ** (-0.5)
        return pl.pallas_call(
            functools.partial(kernel, n_rep, n_tp, scale),
            out_shape=(jax.ShapeDtypeStruct((rows, features), BF16), grad, grad, grad),
            in_specs=[anywhere] * 5,
            out_specs=(vmem,) * 4,
            scratch_shapes=[
                pltpu.VMEM((n_fs, rows, features), BF16),
                pltpu.VMEM((n_fs, rows, features), BF16),
                pltpu.VMEM((features, hidden), BF16),
                pltpu.VMEM((features, hidden), BF16),
                pltpu.VMEM((features, hidden), BF16),
                pltpu.VMEM((features, both), BF16),
                pltpu.VMEM((features, both), BF16),
                pltpu.VMEM((both, hidden), BF16),
                pltpu.VMEM((both, hidden), BF16),
                pltpu.VMEM((both, hidden), BF16),
                pltpu.VMEM((n_fs, rows, features), BF16),
                pltpu.VMEM((n_fs - 1, rows, features), BF16),
                pltpu.VMEM(hops + (span, hidden // 2), BF16),
                pltpu.VMEM(hops + (span, hidden // 2), BF16),
                dma((5,)),
                dma((6,)),
                dma((6,)),
                dma((n_fs, 5)),
                dma((n_fs, 5)),
                dma((n_fs - 1,)),
                dma((n_fs - 1,)),
                dma(hops),
                dma(hops),
            ],
            compiler_params=pltpu.CompilerParams(
                collective_id=0, has_side_effects=True, vmem_limit_bytes=60 * 1024 * 1024
            ),
        )(tokens, cotangent, gate_weight, up_weight, down_weight_t)

    return jax.shard_map(
        on_device,
        mesh=mesh,
        in_specs=(
            P(("rep", "fs", "tp"), None),
            P(("rep", "fs", "tp"), None),
            P(None, "fs"),
            P(None, "fs"),
            P(None, "fs"),
        ),
        out_specs=(
            P(("rep", "fs", "tp"), None),
            P(("rep", "tp"), "fs"),
            P(("rep", "tp"), "fs"),
            P(("rep", "tp"), "fs"),
        ),
        check_vma=False,
    )
```
